32 devices in a mesh: sp: 4 (over z), dp: 8 (over y, x, core).
Axes of the slice: x: 2, y: 2, z: 4, core: 2. Of those that a mesh axis runs over, the one named last changes fastest.
Arguments:
- query_latent: bfloat16 [8, 512, 768], P('dp', 'sp'), may hold values from -6 to 6
- keyvalue_latent: bfloat16 [8, 512, 512], P('dp', 'sp'), may hold values from -6 to 6
- rope_key: bfloat16 [8, 512, 32], P('dp', 'sp'), may hold values from -150 to 150
- query_gain: float32 [768], replicated, may hold values from 0.1 to 1.9
- keyvalue_gain: float32 [512], replicated, may hold values from 0.1 to 1.9
- narrow_query: bfloat16 [768, 384], P('dp'), may hold values from -0.21875 to 0.21875
- broad_query: bfloat16 [768, 640], P('dp'), may hold values from -0.21875 to 0.21875
- narrow_key: bfloat16 [512, 256], P('dp'), may hold values from -0.25 to 0.25
- narrow_value: bfloat16 [512, 256], P('dp'), may hold values from -0.25 to 0.25
- broad_key: bfloat16 [512, 512], P('dp'), may hold values from -0.25 to 0.25
- broad_value: bfloat16 [512, 256], P('dp'), may hold values from -0.25 to 0.25
Outputs:
- narrow_mixed: bfloat16 [8, 512, 256], P('dp', 'sp')
- broad_mixed: bfloat16 [8, 512, 256], P('dp', 'sp')
The draws below stay inside these ranges and needn't reach their ends.
All inputs are finite; a program needn't handle non-finite values.
Results may differ from the reference program's by a relative error of at most 0.014.
The reference program's roundings to bfloat16 on the way count: a program that leaves them out, or rounds other values in their place, can miss the bound.
Values may be sent and summed in bfloat16 or wider, within the bound.
No kernel may reach another device: no remote copies, remote signals or barrier semaphores. Data moves between devices by JAX's collectives and lax.ppermute only.
A program may use at most 64 MiB of HBM per device.

```python
import jax
import jax.numpy as jnp
from jax import lax

QUERY_RANK = 768
PAIR_RANK = 512
PLAIN_NARROW = 64
PLAIN_BROAD = 128
ROTARY = 32
VALUE_SIZE = 64
HEADS = 4
LENGTH = 512
SEQS = 8


def draw_rope_key(key, part):
    base_key = jax.random.fold_in(key, 11)
    values = jnp.clip(jax.random.normal(base_key, (SEQS, LENGTH, ROTARY), jnp.float32), -6.0, 6.0)
    return values.astype(jnp.bfloat16)


def level_of(key, shape, split, smallest, high):
    loudness = 1.0
    for position, shards_of in split:
        draws = jax.random.uniform(jax.random.fold_in(jax.random.fold_in(key, 6), position), (shards_of,), jnp.float32, smallest / len(split), high / len(split))
        loudness = loudness * jnp.repeat(jnp.exp(draws), shape[position] // shards_of).reshape((-1,) + (1,) * (len(shape) - 1 - position))
    return loudness


def normal_values(rng, extent, spread, limit, shards=(), held_as=jnp.bfloat16):
    array = spread * jax.random.normal(rng, extent, jnp.float32)
    if shards:
        array = array * level_of(rng, extent, shards, -0.22, 0.18)
    return jnp.clip(array, -limit, limit).astype(held_as)


def setup_inputs(seed: int = 0) -> dict:
    arg_keys = jax.random.split(jax.random.key(seed), 12)
    return {
        "query_latent": normal_values(arg_keys[0], (SEQS, LENGTH, QUERY_RANK), 1.0, 6.0, ((0, 8), (1, 4))),
        "keyvalue_latent": normal_values(arg_keys[1], (SEQS, LENGTH, PAIR_RANK), 1.0, 6.0, ((0, 8), (1, 4))),
        "rope_key": draw_rope_key(jax.random.fold_in(arg_keys[11], 71), 0),
        "query_gain": jnp.clip(1.0 + 0.18 * jax.random.normal(arg_keys[3], (QUERY_RANK,), jnp.float32), 0.1, 1.9),
        "keyvalue_gain": jnp.clip(1.0 + 0.18 * jax.random.normal(arg_keys[4], (PAIR_RANK,), jnp.float32), 0.1, 1.9),
        "narrow_query": normal_values(arg_keys[5], (QUERY_RANK, HEADS * (PLAIN_NARROW + ROTARY)), QUERY_RANK ** -0.5, 0.21875, ((0, 8),)),
        "broad_query": normal_values(arg_keys[6], (QUERY_RANK, HEADS * (PLAIN_BROAD + ROTARY)), QUERY_RANK ** -0.5, 0.21875, ((0, 8),)),
        "narrow_key": normal_values(arg_keys[7], (PAIR_RANK, HEADS * PLAIN_NARROW), PAIR_RANK ** -0.5, 0.25, ((0, 8),)),
        "narrow_value": normal_values(arg_keys[8], (PAIR_RANK, HEADS * VALUE_SIZE), PAIR_RANK ** -0.5, 0.25, ((0, 8),)),
        "broad_key": normal_values(arg_keys[9], (PAIR_RANK, HEADS * PLAIN_BROAD), PAIR_RANK ** -0.5, 0.25, ((0, 8),)),
        "broad_value": normal_values(arg_keys[10], (PAIR_RANK, HEADS * VALUE_SIZE), PAIR_RANK ** -0.5, 0.25, ((0, 8),)),
    }


EPSILON = 1e-06
ROTARY_BASE = 10000.0

def normalize(latent, gain_row):
    values = latent.astype(jnp.float32)
    scaled = values * lax.rsqrt(lax.optimization_barrier(jnp.mean(values * values, axis=-1, keepdims=True)) + EPSILON)
    return (scaled * gain_row.astype(jnp.float32)).astype(jnp.bfloat16)

def rotate(values, positions):
    halfway = ROTARY // 2
    frequency = ROTARY_BASE ** (-jnp.arange(halfway, dtype=jnp.float32) / halfway)
    angles = positions[:, None] * frequency[None, :]
    cosine = jnp.cos(angles)[:, None, :]
    sine_part = jnp.sin(angles)[:, None, :]
    width = values.shape[-1]
    plain_part = values[..., :width - ROTARY]
    first_half = values[..., width - ROTARY:width - halfway]
    second_half = values[..., width - halfway:]
    return jnp.concatenate([plain_part, first_half * cosine - second_half * sine_part, first_half * sine_part + second_half * cosine], axis=-1)

def attend_group(queries, keys_plain, values, rope_keys, factor):

    def one_head(members):
        query_head, key_head, value_head = members
        key_whole = jnp.concatenate([key_head, rope_keys], axis=1)
        scores = jnp.dot(query_head, key_whole.T, preferred_element_type=jnp.float32) * factor
        shifted = jnp.exp(scores - lax.optimization_barrier(jnp.max(scores, axis=-1, keepdims=True)))
        totals = lax.optimization_barrier(jnp.sum(shifted, axis=-1, keepdims=True))
        mixed = jnp.dot(shifted.astype(jnp.bfloat16), value_head, preferred_element_type=jnp.float32)
        return (mixed / totals).astype(jnp.bfloat16)
    stacked = lax.map(one_head, (jnp.swapaxes(queries, 0, 1), jnp.swapaxes(keys_plain, 0, 1), jnp.swapaxes(values, 0, 1)))
    return jnp.swapaxes(stacked, 0, 1)

def group_norm(attended):
    flattened = attended.reshape(attended.shape[0], -1).astype(jnp.float32)
    scaled = flattened * lax.rsqrt(lax.optimization_barrier(jnp.mean(flattened * flattened, axis=-1, keepdims=True)) + EPSILON)
    return scaled.astype(jnp.bfloat16)

def reference(query_latent, keyvalue_latent, rope_key, query_gain, keyvalue_gain, narrow_query, broad_query, narrow_key, narrow_value, broad_key, broad_value):

    def one_sequence(members):
        query_rows, pair_rows, rope_rows = members
        length = query_rows.shape[0]
        positions = jnp.arange(length).astype(jnp.float32)
        query_normed = normalize(query_rows, query_gain)
        pair_normed = normalize(pair_rows, keyvalue_gain)
        rope_keys = rotate(rope_rows.astype(jnp.float32)[:, None, :], positions)[:, 0, :].astype(jnp.bfloat16)
        width_narrow = PLAIN_NARROW + ROTARY
        width_broad = PLAIN_BROAD + ROTARY
        query_first = rotate(jnp.dot(query_normed, narrow_query, preferred_element_type=jnp.float32).reshape(length, HEADS, width_narrow), positions).astype(jnp.bfloat16)
        query_second = rotate(jnp.dot(query_normed, broad_query, preferred_element_type=jnp.float32).reshape(length, HEADS, width_broad), positions).astype(jnp.bfloat16)
        key_first = jnp.dot(pair_normed, narrow_key, preferred_element_type=jnp.float32).astype(jnp.bfloat16).reshape(length, HEADS, PLAIN_NARROW)
        value_first = jnp.dot(pair_normed, narrow_value, preferred_element_type=jnp.float32).astype(jnp.bfloat16).reshape(length, HEADS, VALUE_SIZE)
        key_second = jnp.dot(pair_normed, broad_key, preferred_element_type=jnp.float32).astype(jnp.bfloat16).reshape(length, HEADS, PLAIN_BROAD)
        value_second = jnp.dot(pair_normed, broad_value, preferred_element_type=jnp.float32).astype(jnp.bfloat16).reshape(length, HEADS, VALUE_SIZE)
        mixed_first = attend_group(query_first, key_first, value_first, rope_keys, width_narrow ** (-0.5))
        mixed_second = attend_group(query_second, key_second, value_second, rope_keys, width_broad ** (-0.5))
        return (group_norm(mixed_first), group_norm(mixed_second))
    narrow_mixed, broad_mixed = lax.map(one_sequence, (query_latent, keyvalue_latent, rope_key))
    return (narrow_mixed, broad_mixed)
```

```python
import functools

import jax
import jax.numpy as jnp
from jax import lax
from jax.experimental import pallas as pl
from jax.experimental.pallas import tpu as pltpu
from jax.sharding import PartitionSpec as P

PLAIN_NARROW = 64
PLAIN_BROAD = 128
ROTARY = 32
VALUE_SIZE = 64


EPSILON = 1e-06
ROTARY_BASE = 10000.0


def normalize(latent, gain_row):
    values = latent.astype(jnp.float32)
    scaled = values * lax.rsqrt(jnp.mean(values * values, axis=-1, keepdims=True) + EPSILON)
    return (scaled * gain_row).astype(jnp.bfloat16)


def rotate(values, positions):
    halfway = ROTARY // 2
    frequency = ROTARY_BASE ** (-jnp.arange(halfway, dtype=jnp.float32) / halfway)
    angles = positions[:, None] * frequency[None, :]
    cosine = jnp.cos(angles)[:, None, :]
    sine_part = jnp.sin(angles)[:, None, :]
    width = values.shape[-1]
    plain_part = values[..., : width - ROTARY]
    first_half = values[..., width - ROTARY : width - halfway]
    second_half = values[..., width - halfway :]
    return jnp.concatenate(
        [
            plain_part,
            first_half * cosine - second_half * sine_part,
            first_half * sine_part + second_half * cosine,
        ],
        axis=-1,
    )


def make_fold(latent, pieces):
    return tuple(
        (jnp.dot(latent, weight_rows, preferred_element_type=jnp.float32) for weight_rows in pieces)
    )


def arrange(sums, width, positions, groups, with_rotary):
    row_count = positions.shape[0]
    shaped = sums.reshape(row_count, -1, width)
    if with_rotary:
        shaped = rotate(shaped, positions)
    shaped = shaped.astype(jnp.bfloat16)
    return shaped.reshape(row_count, groups, shaped.shape[1] // groups, width)


def attend_group(queries, keys_plain, values, rope_keys, factor):
    length = queries.shape[0]
    block_rows = 512
    key_whole = jnp.concatenate([keys_plain[:, 0, :], rope_keys], axis=1)
    value_head = values[:, 0, :]

    def one_block(query_block):
        scores = (
            jnp.einsum("qd,kd->qk", query_block, key_whole, preferred_element_type=jnp.float32)
            * factor
        )
        shifted = jnp.exp(scores - jnp.max(scores, axis=-1, keepdims=True))
        totals = jnp.sum(shifted, axis=-1, keepdims=True)
        mixed = jnp.dot(
            shifted.astype(jnp.bfloat16), value_head, preferred_element_type=jnp.float32
        )
        return (mixed / totals).astype(jnp.bfloat16)

    blocks = lax.map(one_block, queries[:, 0, :].reshape(length // block_rows, block_rows, -1))
    results = [blocks.reshape(length, -1)]
    return jnp.stack(results, axis=1)


def attend_both(members, rope_keys):
    query_first, key_first, value_first, query_second, key_second, value_second = members
    mixed_first = attend_group(
        query_first[:, 0],
        key_first[:, 0],
        value_first[:, 0],
        rope_keys,
        (PLAIN_NARROW + ROTARY) ** (-0.5),
    )
    mixed_second = attend_group(
        query_second[:, 0],
        key_second[:, 0],
        value_second[:, 0],
        rope_keys,
        (PLAIN_BROAD + ROTARY) ** (-0.5),
    )
    return (mixed_first[:, None], mixed_second[:, None])


def finish(mixed):
    flattened = mixed.reshape(mixed.shape[0], -1).astype(jnp.float32)
    scaled = flattened * lax.rsqrt(
        jnp.mean(flattened * flattened, axis=-1, keepdims=True) + EPSILON
    )
    return scaled.astype(jnp.bfloat16)[None]


def by_heads(
    query_latent,
    keyvalue_latent,
    rope_key,
    query_gain,
    keyvalue_gain,
    narrow_query,
    broad_query,
    narrow_key,
    narrow_value,
    broad_key,
    broad_value,
):
    tokens = query_latent.shape[1]
    spread = lax.axis_size("sp")
    device_index = lax.axis_index("sp")
    width_narrow = PLAIN_NARROW + ROTARY
    width_broad = PLAIN_BROAD + ROTARY
    query_normed = normalize(query_latent[0], query_gain)
    pair_normed = normalize(keyvalue_latent[0], keyvalue_gain)
    own_positions = (device_index * tokens + jnp.arange(tokens, dtype=jnp.int32)).astype(
        jnp.float32
    )
    rope_own = rotate(rope_key[0].astype(jnp.float32)[:, None, :], own_positions)[:, 0, :].astype(
        jnp.bfloat16
    )
    query_all, pair_all, rope_all = (
        lax.all_gather(query_normed, "sp", axis=0, tiled=True),
        lax.all_gather(pair_normed, "sp", axis=0, tiled=True),
        lax.all_gather(rope_own, "sp", axis=0, tiled=True),
    )
    length = tokens * spread
    all_positions = jnp.arange(length, dtype=jnp.int32).astype(jnp.float32)

    def own_columns(weight, width):
        count = weight.shape[1] // (width * spread)
        return lax.dynamic_slice_in_dim(weight, device_index * count * width, count * width, 1)

    own_narrow_query = own_columns(narrow_query, width_narrow)
    own_broad_query = own_columns(broad_query, width_broad)
    own_narrow_key = own_columns(narrow_key, PLAIN_NARROW)
    own_narrow_value = own_columns(narrow_value, VALUE_SIZE)
    own_broad_key = own_columns(broad_key, PLAIN_BROAD)
    own_broad_value = own_columns(broad_value, VALUE_SIZE)
    query_sums = make_fold(
        query_all,
        (
            lax.all_gather(own_narrow_query, "dp", axis=0, tiled=True),
            lax.all_gather(own_broad_query, "dp", axis=0, tiled=True),
        ),
    )
    pair_sums = make_fold(
        pair_all,
        (
            lax.all_gather(own_narrow_key, "dp", axis=0, tiled=True),
            lax.all_gather(own_narrow_value, "dp", axis=0, tiled=True),
            lax.all_gather(own_broad_key, "dp", axis=0, tiled=True),
            lax.all_gather(own_broad_value, "dp", axis=0, tiled=True),
        ),
    )
    members = (
        arrange(query_sums[0], width_narrow, all_positions, 1, True),
        arrange(pair_sums[0], PLAIN_NARROW, all_positions, 1, False),
        arrange(pair_sums[1], VALUE_SIZE, all_positions, 1, False),
        arrange(query_sums[1], width_broad, all_positions, 1, True),
        arrange(pair_sums[2], PLAIN_BROAD, all_positions, 1, False),
        arrange(pair_sums[3], VALUE_SIZE, all_positions, 1, False),
    )
    mixed_first, mixed_second = attend_both(members, rope_all)
    back_first, back_second = (
        lax.all_to_all(mixed_first, "sp", split_axis=0, concat_axis=1, tiled=True),
        lax.all_to_all(mixed_second, "sp", split_axis=0, concat_axis=1, tiled=True),
    )
    return (finish(back_first), finish(back_second))


VMEM = pl.BlockSpec(memory_space=pltpu.VMEM)


def exchange(array, axis, distance):
    size = lax.axis_size(axis)
    return lax.ppermute(array, axis, [(i, i ^ distance) for i in range(size)])


def scale_rows(values, gain):
    return (
        values * lax.rsqrt(jnp.mean(values * values, axis=-1, keepdims=True) + EPSILON) * gain
    )


def pack_kernel(
    latent, rope, narrow_key, narrow_value, broad_key, broad_value, narrow_query, broad_query,
    latent_out, pair_out, query_out,
):
    tokens, rank = latent.shape
    latent_out[:tokens, :] = latent[...]
    pieces = rank // ROTARY
    rows = tokens // pieces
    wide = rope[...].astype(jnp.float32)
    wide = jnp.concatenate([wide[rows * j : rows * (j + 1), :] for j in range(pieces)], axis=1)
    latent_out[tokens:, :] = wide.astype(jnp.bfloat16)
    start = 0
    for piece in (narrow_key, narrow_value, broad_key, broad_value):
        pair_out[:, start : start + piece.shape[1]] = piece[...]
        start += piece.shape[1]
    start = 0
    for piece in (narrow_query, broad_query):
        query_out[:, start : start + piece.shape[1]] = piece[...]
        start += piece.shape[1]


def gather_rows(blocks, weight):
    me = lax.axis_index("dp")
    for distance, block in enumerate(blocks):
        rows = block.shape[0]
        weight[pl.ds(pl.multiple_of((me ^ distance) * rows, rows), rows), :] = block[...]


def pair_kernel(parts, shares, heads, *refs):
    latents, blocks = refs[:parts], refs[parts : parts + shares]
    gain, cosine, sine, narrow_keys, narrow_values, broad_keys, broad_values, weight = refs[
        parts + shares :
    ]
    gather_rows(blocks, weight)
    rank = weight.shape[0]
    half = ROTARY // 2
    narrow, broad, value = PLAIN_NARROW * heads, PLAIN_BROAD * heads, VALUE_SIZE * heads
    for part in range(parts):
        latent = latents[part]
        rows = latent.shape[0] * rank // (rank + ROTARY)
        own = slice(rows * part, rows * (part + 1))
        normed = scale_rows(latent[:rows, :].astype(jnp.float32), gain[...]).astype(jnp.bfloat16)
        wide = latent[rows:, :].astype(jnp.float32)
        rope = jnp.concatenate(
            [wide[:, ROTARY * j : ROTARY * (j + 1)] for j in range(rank // ROTARY)], axis=0
        )
        swapped = jnp.concatenate([rope[:, half:], rope[:, :half]], axis=1)
        rope = (rope * cosine[own, :ROTARY] + swapped * sine[own, :ROTARY]).astype(jnp.bfloat16)
        sums = jnp.dot(normed, weight[...], preferred_element_type=jnp.float32).astype(
            jnp.bfloat16
        )
        for head in range(heads):
            start = PLAIN_NARROW * head
            narrow_keys[head, own, :PLAIN_NARROW] = sums[:, start : start + PLAIN_NARROW]
            narrow_keys[head, own, PLAIN_NARROW:] = rope
            start = narrow + value + PLAIN_BROAD * head
            broad_keys[head, own, :PLAIN_BROAD] = sums[:, start : start + PLAIN_BROAD]
            broad_keys[head, own, PLAIN_BROAD:] = rope
        narrow_values[own, :] = sums[:, narrow : narrow + value]
        broad_values[own, :] = sums[:, narrow + value + broad :]


def attend_heads(queries, keys, values, width, out):
    heads = keys.shape[0]
    lanes = 2 * VALUE_SIZE
    low = lax.broadcasted_iota(jnp.int32, (1, lanes), 1) < VALUE_SIZE
    attended = []
    for pair in range(heads // 2):
        value = values[:, lanes * pair : lanes * (pair + 1)]
        results = []
        for head in (2 * pair, 2 * pair + 1):
            query = queries[:, width * head : width * (head + 1)]
            scores = lax.dot_general(
                query, keys[head], (((1,), (1,)), ((), ())), preferred_element_type=jnp.float32
            ) * (width ** (-0.5))
            shifted = jnp.exp(scores - jnp.max(scores, axis=-1, keepdims=True))
            totals = jnp.sum(shifted, axis=-1, keepdims=True)
            mixed = jnp.dot(
                shifted.astype(jnp.bfloat16), value, preferred_element_type=jnp.float32
            )
            results.append(mixed / totals)
        attended.append(jnp.where(low, *results).astype(jnp.bfloat16).astype(jnp.float32))
    attended = jnp.concatenate(attended, axis=1)
    out[...] = scale_rows(attended, 1.0).astype(jnp.bfloat16)


def turn(sums, width, cosine, sine):
    lanes = cosine.shape[1]
    lane = lax.broadcasted_iota(jnp.int32, (1, lanes), 1)
    first = lane % ROTARY < ROTARY // 2
    turned = []
    for start in range(0, sums.shape[1], lanes):
        tile = sums[:, start : start + lanes]
        partner = jnp.where(
            first, pltpu.roll(tile, lanes - ROTARY // 2, 1), pltpu.roll(tile, ROTARY // 2, 1)
        )
        rotary = (lane + start) % width >= width - ROTARY
        turned.append(jnp.where(rotary, tile * cosine + partner * sine, tile))
    return jnp.concatenate(turned, axis=1).astype(jnp.bfloat16)


def query_kernel(shares, heads, *refs):
    blocks = refs[:shares]
    latent, gain, cosine, sine, narrow_keys, narrow_values, broad_keys, broad_values = refs[
        shares : shares + 8
    ]
    narrow_out, broad_out, weight = refs[shares + 8 :]
    gather_rows(blocks, weight)
    normed = scale_rows(latent[...].astype(jnp.float32), gain[...]).astype(jnp.bfloat16)
    sums = jnp.dot(normed, weight[...], preferred_element_type=jnp.float32)
    tokens = latent.shape[0]
    cosine, sine = cosine[:tokens, :], sine[:tokens, :]
    width = PLAIN_NARROW + ROTARY
    narrow = turn(sums[:, : width * heads], width, cosine, sine)
    attend_heads(narrow, narrow_keys, narrow_values, width, narrow_out)
    split = width * heads
    width = PLAIN_BROAD + ROTARY
    broad = turn(sums[:, split:], width, cosine, sine)
    attend_heads(broad, broad_keys, broad_values, width, broad_out)


def by_tokens(
    query_latent,
    keyvalue_latent,
    rope_key,
    query_gain,
    keyvalue_gain,
    narrow_query,
    broad_query,
    narrow_key,
    narrow_value,
    broad_key,
    broad_value,
):
    shape = jax.ShapeDtypeStruct
    spread, shares = lax.axis_size("sp"), lax.axis_size("dp")
    tokens, pair_rank = keyvalue_latent.shape[1:]
    query_rank = query_latent.shape[2]
    heads = narrow_value.shape[1] // VALUE_SIZE
    values = VALUE_SIZE * heads
    pair_width = narrow_key.shape[1] + broad_key.shape[1] + 2 * values
    query_width = narrow_query.shape[1] + broad_query.shape[1]
    length = tokens * spread

    packed, pair_rows, query_rows = pl.pallas_call(
        pack_kernel,
        out_shape=(
            shape((tokens + tokens * ROTARY // pair_rank, pair_rank), jnp.bfloat16),
            shape((pair_rank // shares, pair_width), jnp.bfloat16),
            shape((query_rank // shares, query_width), jnp.bfloat16),
        ),
        in_specs=[VMEM] * 8,
        out_specs=(VMEM,) * 3,
    )(
        keyvalue_latent[0], rope_key[0], narrow_key, narrow_value, broad_key, broad_value,
        narrow_query, broad_query,
    )

    def from_chips(array):
        return [array] + [exchange(array, "dp", k) for k in range(2, shares, 2)]

    def with_partner(arrays):
        both = []
        for array in arrays:
            both += [array, exchange(array, "dp", 1)]
        return both

    pair_blocks = from_chips(pair_rows)
    query_blocks = from_chips(query_rows)
    latents = [packed] + [exchange(packed, "sp", k) for k in range(1, spread)]
    pair_blocks, query_blocks = with_partner(pair_blocks), with_partner(query_blocks)

    lane = jnp.arange(4 * ROTARY, dtype=jnp.int32)
    half = ROTARY // 2
    frequency = ROTARY_BASE ** (-(lane % half).astype(jnp.float32) / half)
    place = jnp.arange(length, dtype=jnp.int32)
    places = (lax.axis_index("sp") ^ (place // tokens)) * tokens + place % tokens
    angles = places.astype(jnp.float32)[:, None] * frequency[None, :]
    cosine = jnp.cos(angles)
    sine = jnp.where(lane % ROTARY < half, -1.0, 1.0)[None, :] * jnp.sin(angles)

    keys_and_values = pl.pallas_call(
        functools.partial(pair_kernel, spread, shares, heads),
        out_shape=(
            shape((heads, length, PLAIN_NARROW + ROTARY), jnp.bfloat16),
            shape((length, values), jnp.bfloat16),
            shape((heads, length, PLAIN_BROAD + ROTARY), jnp.bfloat16),
            shape((length, values), jnp.bfloat16),
        ),
        in_specs=[VMEM] * (spread + shares + 3),
        out_specs=(VMEM,) * 4,
        scratch_shapes=[pltpu.VMEM((pair_rank, pair_width), jnp.bfloat16)],
    )(*latents, *pair_blocks, keyvalue_gain[None, :], cosine, sine)

    narrow, broad = pl.pallas_call(
        functools.partial(query_kernel, shares, heads),
        out_shape=(shape((tokens, values), jnp.bfloat16),) * 2,
        in_specs=[VMEM] * (shares + 8),
        out_specs=(VMEM,) * 2,
        scratch_shapes=[pltpu.VMEM((query_rank, query_width), jnp.bfloat16)],
    )(*query_blocks, query_latent[0], query_gain[None, :], cosine, sine, *keys_and_values)
    return narrow[None], broad[None]


def solution(mesh):
    small = mesh.shape["dp"] == 8 and mesh.shape["sp"] == 4
    on_device = by_tokens if small else by_heads

    in_specs = (
        P("dp", "sp", None),
        P("dp", "sp", None),
        P("dp", "sp", None),
        P(),
        P(),
        P("dp", None),
        P("dp", None),
        P("dp", None),
        P("dp", None),
        P("dp", None),
        P("dp", None),
    )
    out_specs = (P("dp", "sp", None), P("dp", "sp", None))
    return jax.shard_map(
        on_device, mesh=mesh, in_specs=in_specs, out_specs=out_specs, check_vma=False
    )
```

```python
import functools

import jax
import jax.numpy as jnp
from jax import lax
from jax.experimental import pallas as pl
from jax.experimental.pallas import tpu as pltpu
from jax.sharding import PartitionSpec as P

PLAIN_NARROW = 64
PLAIN_BROAD = 128
ROTARY = 32
VALUE_SIZE = 64


EPSILON = 1e-06
ROTARY_BASE = 10000.0


def normalize(latent, gain_row):
    values = latent.astype(jnp.float32)
    scaled = values * lax.rsqrt(jnp.mean(values * values, axis=-1, keepdims=True) + EPSILON)
    return (scaled * gain_row).astype(jnp.bfloat16)


def rotate(values, positions):
    halfway = ROTARY // 2
    frequency = ROTARY_BASE ** (-jnp.arange(halfway, dtype=jnp.float32) / halfway)
    angles = positions[:, None] * frequency[None, :]
    cosine = jnp.cos(angles)[:, None, :]
    sine_part = jnp.sin(angles)[:, None, :]
    width = values.shape[-1]
    plain_part = values[..., : width - ROTARY]
    first_half = values[..., width - ROTARY : width - halfway]
    second_half = values[..., width - halfway :]
    return jnp.concatenate(
        [
            plain_part,
            first_half * cosine - second_half * sine_part,
            first_half * sine_part + second_half * cosine,
        ],
        axis=-1,
    )


def make_fold(latent, pieces):
    return tuple(
        (jnp.dot(latent, weight_rows, preferred_element_type=jnp.float32) for weight_rows in pieces)
    )


def arrange(sums, width, positions, groups, with_rotary):
    row_count = positions.shape[0]
    shaped = sums.reshape(row_count, -1, width)
    if with_rotary:
        shaped = rotate(shaped, positions)
    shaped = shaped.astype(jnp.bfloat16)
    return shaped.reshape(row_count, groups, shaped.shape[1] // groups, width)


def attend_group(queries, keys_plain, values, rope_keys, factor):
    length = queries.shape[0]
    block_rows = 512
    key_whole = jnp.concatenate([keys_plain[:, 0, :], rope_keys], axis=1)
    value_head = values[:, 0, :]

    def one_block(query_block):
        scores = (
            jnp.einsum("qd,kd->qk", query_block, key_whole, preferred_element_type=jnp.float32)
            * factor
        )
        shifted = jnp.exp(scores - jnp.max(scores, axis=-1, keepdims=True))
        totals = jnp.sum(shifted, axis=-1, keepdims=True)
        mixed = jnp.dot(
            shifted.astype(jnp.bfloat16), value_head, preferred_element_type=jnp.float32
        )
        return (mixed / totals).astype(jnp.bfloat16)

    blocks = lax.map(one_block, queries[:, 0, :].reshape(length // block_rows, block_rows, -1))
    results = [blocks.reshape(length, -1)]
    return jnp.stack(results, axis=1)


def attend_both(members, rope_keys):
    query_first, key_first, value_first, query_second, key_second, value_second = members
    mixed_first = attend_group(
        query_first[:, 0],
        key_first[:, 0],
        value_first[:, 0],
        rope_keys,
        (PLAIN_NARROW + ROTARY) ** (-0.5),
    )
    mixed_second = attend_group(
        query_second[:, 0],
        key_second[:, 0],
        value_second[:, 0],
        rope_keys,
        (PLAIN_BROAD + ROTARY) ** (-0.5),
    )
    return (mixed_first[:, None], mixed_second[:, None])


def finish(mixed):
    flattened = mixed.reshape(mixed.shape[0], -1).astype(jnp.float32)
    scaled = flattened * lax.rsqrt(
        jnp.mean(flattened * flattened, axis=-1, keepdims=True) + EPSILON
    )
    return scaled.astype(jnp.bfloat16)[None]


def by_heads(
    query_latent,
    keyvalue_latent,
    rope_key,
    query_gain,
    keyvalue_gain,
    narrow_query,
    broad_query,
    narrow_key,
    narrow_value,
    broad_key,
    broad_value,
):
    tokens = query_latent.shape[1]
    spread = lax.axis_size("sp")
    device_index = lax.axis_index("sp")
    width_narrow = PLAIN_NARROW + ROTARY
    width_broad = PLAIN_BROAD + ROTARY
    query_normed = normalize(query_latent[0], query_gain)
    pair_normed = normalize(keyvalue_latent[0], keyvalue_gain)
    own_positions = (device_index * tokens + jnp.arange(tokens, dtype=jnp.int32)).astype(
        jnp.float32
    )
    rope_own = rotate(rope_key[0].astype(jnp.float32)[:, None, :], own_positions)[:, 0, :].astype(
        jnp.bfloat16
    )
    query_all, pair_all, rope_all = (
        lax.all_gather(query_normed, "sp", axis=0, tiled=True),
        lax.all_gather(pair_normed, "sp", axis=0, tiled=True),
        lax.all_gather(rope_own, "sp", axis=0, tiled=True),
    )
    length = tokens * spread
    all_positions = jnp.arange(length, dtype=jnp.int32).astype(jnp.float32)

    def own_columns(weight, width):
        count = weight.shape[1] // (width * spread)
        return lax.dynamic_slice_in_dim(weight, device_index * count * width, count * width, 1)

    own_narrow_query = own_columns(narrow_query, width_narrow)
    own_broad_query = own_columns(broad_query, width_broad)
    own_narrow_key = own_columns(narrow_key, PLAIN_NARROW)
    own_narrow_value = own_columns(narrow_value, VALUE_SIZE)
    own_broad_key = own_columns(broad_key, PLAIN_BROAD)
    own_broad_value = own_columns(broad_value, VALUE_SIZE)
    query_sums = make_fold(
        query_all,
        (
            lax.all_gather(own_narrow_query, "dp", axis=0, tiled=True),
            lax.all_gather(own_broad_query, "dp", axis=0, tiled=True),
        ),
    )
    pair_sums = make_fold(
        pair_all,
        (
            lax.all_gather(own_narrow_key, "dp", axis=0, tiled=True),
            lax.all_gather(own_narrow_value, "dp", axis=0, tiled=True),
            lax.all_gather(own_broad_key, "dp", axis=0, tiled=True),
            lax.all_gather(own_broad_value, "dp", axis=0, tiled=True),
        ),
    )
    members = (
        arrange(query_sums[0], width_narrow, all_positions, 1, True),
        arrange(pair_sums[0], PLAIN_NARROW, all_positions, 1, False),
        arrange(pair_sums[1], VALUE_SIZE, all_positions, 1, False),
        arrange(query_sums[1], width_broad, all_positions, 1, True),
        arrange(pair_sums[2], PLAIN_BROAD, all_positions, 1, False),
        arrange(pair_sums[3], VALUE_SIZE, all_positions, 1, False),
    )
    mixed_first, mixed_second = attend_both(members, rope_all)
    back_first, back_second = (
        lax.all_to_all(mixed_first, "sp", split_axis=0, concat_axis=1, tiled=True),
        lax.all_to_all(mixed_second, "sp", split_axis=0, concat_axis=1, tiled=True),
    )
    return (finish(back_first), finish(back_second))


VMEM = pl.BlockSpec(memory_space=pltpu.VMEM)
SMALL = pltpu.CompilerParams(vmem_limit_bytes=16 * 2**20)


def exchange(array, axis, distance):
    size = lax.axis_size(axis)
    return lax.ppermute(array, axis, [(i, i ^ distance) for i in range(size)])


def scale_rows(values, gain):
    return (
        values * lax.rsqrt(jnp.mean(values * values, axis=-1, keepdims=True) + EPSILON) * gain
    )


def pack_kernel(
    latent, rope, narrow_key, narrow_value, broad_key, broad_value, narrow_query, broad_query,
    latent_out, pair_out, query_out, semaphores,
):
    tokens, rank = latent.shape
    pieces = rank // tokens
    rows = rope.shape[0] // pieces
    copies = [(latent, latent_out.at[:tokens, :])]
    for j in range(pieces):
        copies.append(
            (
                rope.at[rows * j : rows * (j + 1), :],
                latent_out.at[tokens:, tokens * j : tokens * (j + 1)],
            )
        )
    start = 0
    for piece in (narrow_key, narrow_value, broad_key, broad_value):
        copies.append((piece, pair_out.at[:, start : start + piece.shape[1]]))
        start += piece.shape[1]
    start = 0
    for piece in (narrow_query, broad_query):
        copies.append((piece, query_out.at[:, start : start + piece.shape[1]]))
        start += piece.shape[1]
    copies = [
        pltpu.make_async_copy(source, target, semaphores.at[i])
        for i, (source, target) in enumerate(copies)
    ]
    for copy in copies:
        copy.start()
    for copy in copies:
        copy.wait()


def gather_rows(blocks, weight):
    me = lax.axis_index("dp")
    for distance, block in enumerate(blocks):
        rows = block.shape[0]
        weight[pl.ds(pl.multiple_of((me ^ distance) * rows, rows), rows), :] = block[...]


def pair_kernel(parts, shares, heads, *refs):
    latents, blocks = refs[:parts], refs[parts : parts + shares]
    gain, cosine, sine, narrow_keys, narrow_values, broad_keys, broad_values, weight = refs[
        parts + shares :
    ]
    gather_rows(blocks, weight)
    rank = weight.shape[0]
    half = ROTARY // 2
    narrow, broad, value = PLAIN_NARROW * heads, PLAIN_BROAD * heads, VALUE_SIZE * heads
    for part in range(parts):
        latent = latents[part]
        rows = latent.shape[0] * rank // (rank + ROTARY)
        lift = ROTARY * rows // rank
        own = slice(rows * part, rows * (part + 1))
        normed = scale_rows(latent[:rows, :].astype(jnp.float32), gain[...]).astype(jnp.bfloat16)
        wide = latent[rows:, :].astype(jnp.float32)
        rope = jnp.concatenate(
            [wide[:, rows * j : rows * (j + 1)] for j in range(ROTARY // lift)], axis=0
        )
        first, second = rope[:half], rope[half:]
        near, far = cosine[:, own], sine[:, own]
        rope = jnp.concatenate([first * near - second * far, first * far + second * near], axis=0)
        rope = rope.T.astype(jnp.bfloat16)
        sums = jnp.dot(normed, weight[...], preferred_element_type=jnp.float32).astype(
            jnp.bfloat16
        )
        for head in range(heads):
            start = PLAIN_NARROW * head
            narrow_keys[head, own, :PLAIN_NARROW] = sums[:, start : start + PLAIN_NARROW]
            narrow_keys[head, own, PLAIN_NARROW:] = rope
            start = narrow + value + PLAIN_BROAD * head
            broad_keys[head, own, :PLAIN_BROAD] = sums[:, start : start + PLAIN_BROAD]
            broad_keys[head, own, PLAIN_BROAD:] = rope
        narrow_values[own, :] = sums[:, narrow : narrow + value]
        broad_values[own, :] = sums[:, narrow + value + broad :]


def attend_heads(queries, keys, values, width, out):
    heads = keys.shape[0]
    lanes = 2 * VALUE_SIZE
    low = lax.broadcasted_iota(jnp.int32, (1, lanes), 1) < VALUE_SIZE
    attended = []
    for pair in range(heads // 2):
        value = values[:, lanes * pair : lanes * (pair + 1)]
        results = []
        for head in (2 * pair, 2 * pair + 1):
            query = queries[:, width * head : width * (head + 1)]
            scores = lax.dot_general(
                query, keys[head], (((1,), (1,)), ((), ())), preferred_element_type=jnp.float32
            ) * (width ** (-0.5))
            shifted = jnp.exp(scores - jnp.max(scores, axis=-1, keepdims=True))
            totals = jnp.sum(shifted, axis=-1, keepdims=True)
            mixed = jnp.dot(
                shifted.astype(jnp.bfloat16), value, preferred_element_type=jnp.float32
            )
            results.append(mixed / totals)
        attended.append(jnp.where(low, *results).astype(jnp.bfloat16).astype(jnp.float32))
    attended = jnp.concatenate(attended, axis=1)
    out[...] = scale_rows(attended, 1.0).astype(jnp.bfloat16)


def turn(sums, width, cosine, sine):
    lanes = cosine.shape[1]
    lane = lax.broadcasted_iota(jnp.int32, (1, lanes), 1)
    first = lane % ROTARY < ROTARY // 2
    turned = []
    for start in range(0, sums.shape[1], lanes):
        tile = sums[:, start : start + lanes]
        partner = jnp.where(
            first, pltpu.roll(tile, lanes - ROTARY // 2, 1), pltpu.roll(tile, ROTARY // 2, 1)
        )
        rotary = (lane + start) % width >= width - ROTARY
        turned.append(jnp.where(rotary, tile * cosine + partner * sine, tile))
    return jnp.concatenate(turned, axis=1).astype(jnp.bfloat16)


def query_kernel(shares, heads, *refs):
    blocks = refs[:shares]
    latent, gain, cosine, sine, narrow_keys, narrow_values, broad_keys, broad_values = refs[
        shares : shares + 8
    ]
    narrow_out, broad_out, weight = refs[shares + 8 :]
    gather_rows(blocks, weight)
    normed = scale_rows(latent[...].astype(jnp.float32), gain[...]).astype(jnp.bfloat16)
    sums = jnp.dot(normed, weight[...], preferred_element_type=jnp.float32)
    cosine, sine = cosine[...], sine[...]
    width = PLAIN_NARROW + ROTARY
    narrow = turn(sums[:, : width * heads], width, cosine, sine)
    attend_heads(narrow, narrow_keys, narrow_values, width, narrow_out)
    split = width * heads
    width = PLAIN_BROAD + ROTARY
    broad = turn(sums[:, split:], width, cosine, sine)
    attend_heads(broad, broad_keys, broad_values, width, broad_out)


def by_tokens(
    query_latent,
    keyvalue_latent,
    rope_key,
    query_gain,
    keyvalue_gain,
    narrow_query,
    broad_query,
    narrow_key,
    narrow_value,
    broad_key,
    broad_value,
):
    shape = jax.ShapeDtypeStruct
    spread, shares = lax.axis_size("sp"), lax.axis_size("dp")
    tokens, pair_rank = keyvalue_latent.shape[1:]
    query_rank = query_latent.shape[2]
    heads = narrow_value.shape[1] // VALUE_SIZE
    values = VALUE_SIZE * heads
    pair_width = narrow_key.shape[1] + broad_key.shape[1] + 2 * values
    query_width = narrow_query.shape[1] + broad_query.shape[1]
    length = tokens * spread

    pieces = pair_rank // tokens
    packed, pair_rows, query_rows = pl.pallas_call(
        pack_kernel,
        out_shape=(
            shape((tokens + ROTARY // pieces, pair_rank), jnp.bfloat16),
            shape((pair_rank // shares, pair_width), jnp.bfloat16),
            shape((query_rank // shares, query_width), jnp.bfloat16),
        ),
        in_specs=[pl.BlockSpec(memory_space=pltpu.HBM)] * 8,
        out_specs=(VMEM,) * 3,
        scratch_shapes=[pltpu.SemaphoreType.DMA((7 + pieces,))],
        compiler_params=SMALL,
    )(
        *(
            pltpu.with_memory_space_constraint(array, pltpu.HBM)
            for array in (
                keyvalue_latent[0], rope_key[0].T, narrow_key, narrow_value, broad_key,
                broad_value, narrow_query, broad_query,
            )
        )
    )

    def from_chips(array):
        return [array] + [exchange(array, "dp", k) for k in range(2, shares, 2)]

    def with_partner(arrays):
        both = []
        for array in arrays:
            both += [array, exchange(array, "dp", 1)]
        return both

    pair_blocks = from_chips(pair_rows)
    query_blocks = from_chips(query_rows)
    latents = [packed] + [exchange(packed, "sp", k) for k in range(1, spread)]
    pair_blocks = with_partner(pair_blocks)

    half = ROTARY // 2
    frequency = ROTARY_BASE ** (-jnp.arange(half, dtype=jnp.float32) / half)
    place = jnp.arange(length, dtype=jnp.int32)
    me = lax.axis_index("sp")
    places = (me ^ (place // tokens)) * tokens + place % tokens
    angles = frequency[:, None] * places.astype(jnp.float32)[None, :]
    key_cosine, key_sine = jnp.cos(angles), jnp.sin(angles)
    lane = jnp.arange(4 * ROTARY, dtype=jnp.int32)
    frequency = ROTARY_BASE ** (-(lane % half).astype(jnp.float32) / half)
    places = me * tokens + jnp.arange(tokens, dtype=jnp.int32)
    angles = places.astype(jnp.float32)[:, None] * frequency[None, :]
    cosine = jnp.cos(angles)
    sine = jnp.where(lane % ROTARY < half, -1.0, 1.0)[None, :] * jnp.sin(angles)

    keys_and_values = pl.pallas_call(
        functools.partial(pair_kernel, spread, shares, heads),
        out_shape=(
            shape((heads, length, PLAIN_NARROW + ROTARY), jnp.bfloat16),
            shape((length, values), jnp.bfloat16),
            shape((heads, length, PLAIN_BROAD + ROTARY), jnp.bfloat16),
            shape((length, values), jnp.bfloat16),
        ),
        in_specs=[VMEM] * (spread + shares + 3),
        out_specs=(VMEM,) * 4,
        compiler_params=SMALL,
        scratch_shapes=[pltpu.VMEM((pair_rank, pair_width), jnp.bfloat16)],
        cost_estimate=pl.CostEstimate(
            flops=2 * length * pair_rank * pair_width, bytes_accessed=0, transcendentals=0
        ),
    )(*latents, *pair_blocks, keyvalue_gain[None, :], key_cosine, key_sine)

    keys_and_values = list(keys_and_values)
    for i in range(1, len(query_blocks)):
        query_blocks[i], keys_and_values[0] = lax.optimization_barrier(
            (query_blocks[i], keys_and_values[0])
        )
    query_blocks = with_partner(query_blocks)

    narrow, broad = pl.pallas_call(
        functools.partial(query_kernel, shares, heads),
        out_shape=(shape((tokens, values), jnp.bfloat16),) * 2,
        in_specs=[VMEM] * (shares + 8),
        out_specs=(VMEM,) * 2,
        compiler_params=SMALL,
        scratch_shapes=[pltpu.VMEM((query_rank, query_width), jnp.bfloat16)],
    )(*query_blocks, query_latent[0], query_gain[None, :], cosine, sine, *keys_and_values)
    return narrow[None], broad[None]


def solution(mesh):
    small = mesh.shape["dp"] == 8 and mesh.shape["sp"] == 4
    on_device = by_tokens if small else by_heads

    in_specs = (
        P("dp", "sp", None),
        P("dp", "sp", None),
        P("dp", "sp", None),
        P(),
        P(),
        P("dp", None),
        P("dp", None),
        P("dp", None),
        P("dp", None),
        P("dp", None),
        P("dp", None),
    )
    out_specs = (P("dp", "sp", None), P("dp", "sp", None))
    return jax.shard_map(
        on_device, mesh=mesh, in_specs=in_specs, out_specs=out_specs, check_vma=False
    )
```

```python
import functools

import jax
import jax.numpy as jnp
from jax import lax
from jax.experimental import pallas as pl
from jax.experimental.pallas import tpu as pltpu
from jax.sharding import PartitionSpec as P

PLAIN_NARROW = 64
PLAIN_BROAD = 128
ROTARY = 32
VALUE_SIZE = 64


EPSILON = 1e-06
ROTARY_BASE = 10000.0


def normalize(latent, gain_row):
    values = latent.astype(jnp.float32)
    scaled = values * lax.rsqrt(jnp.mean(values * values, axis=-1, keepdims=True) + EPSILON)
    return (scaled * gain_row).astype(jnp.bfloat16)


def rotate(values, positions):
    halfway = ROTARY // 2
    frequency = ROTARY_BASE ** (-jnp.arange(halfway, dtype=jnp.float32) / halfway)
    angles = positions[:, None] * frequency[None, :]
    cosine = jnp.cos(angles)[:, None, :]
    sine_part = jnp.sin(angles)[:, None, :]
    width = values.shape[-1]
    plain_part = values[..., : width - ROTARY]
    first_half = values[..., width - ROTARY : width - halfway]
    second_half = values[..., width - halfway :]
    return jnp.concatenate(
        [
            plain_part,
            first_half * cosine - second_half * sine_part,
            first_half * sine_part + second_half * cosine,
        ],
        axis=-1,
    )


def make_fold(latent, pieces):
    return tuple(
        (jnp.dot(latent, weight_rows, preferred_element_type=jnp.float32) for weight_rows in pieces)
    )


def arrange(sums, width, positions, groups, with_rotary):
    row_count = positions.shape[0]
    shaped = sums.reshape(row_count, -1, width)
    if with_rotary:
        shaped = rotate(shaped, positions)
    shaped = shaped.astype(jnp.bfloat16)
    return shaped.reshape(row_count, groups, shaped.shape[1] // groups, width)


def attend_group(queries, keys_plain, values, rope_keys, factor):
    length = queries.shape[0]
    block_rows = 512
    key_whole = jnp.concatenate([keys_plain[:, 0, :], rope_keys], axis=1)
    value_head = values[:, 0, :]

    def one_block(query_block):
        scores = (
            jnp.einsum("qd,kd->qk", query_block, key_whole, preferred_element_type=jnp.float32)
            * factor
        )
        shifted = jnp.exp(scores - jnp.max(scores, axis=-1, keepdims=True))
        totals = jnp.sum(shifted, axis=-1, keepdims=True)
        mixed = jnp.dot(
            shifted.astype(jnp.bfloat16), value_head, preferred_element_type=jnp.float32
        )
        return (mixed / totals).astype(jnp.bfloat16)

    blocks = lax.map(one_block, queries[:, 0, :].reshape(length // block_rows, block_rows, -1))
    results = [blocks.reshape(length, -1)]
    return jnp.stack(results, axis=1)


def attend_both(members, rope_keys):
    query_first, key_first, value_first, query_second, key_second, value_second = members
    mixed_first = attend_group(
        query_first[:, 0],
        key_first[:, 0],
        value_first[:, 0],
        rope_keys,
        (PLAIN_NARROW + ROTARY) ** (-0.5),
    )
    mixed_second = attend_group(
        query_second[:, 0],
        key_second[:, 0],
        value_second[:, 0],
        rope_keys,
        (PLAIN_BROAD + ROTARY) ** (-0.5),
    )
    return (mixed_first[:, None], mixed_second[:, None])


def finish(mixed):
    flattened = mixed.reshape(mixed.shape[0], -1).astype(jnp.float32)
    scaled = flattened * lax.rsqrt(
        jnp.mean(flattened * flattened, axis=-1, keepdims=True) + EPSILON
    )
    return scaled.astype(jnp.bfloat16)[None]


def by_heads(
    query_latent,
    keyvalue_latent,
    rope_key,
    query_gain,
    keyvalue_gain,
    narrow_query,
    broad_query,
    narrow_key,
    narrow_value,
    broad_key,
    broad_value,
):
    tokens = query_latent.shape[1]
    spread = lax.axis_size("sp")
    device_index = lax.axis_index("sp")
    width_narrow = PLAIN_NARROW + ROTARY
    width_broad = PLAIN_BROAD + ROTARY
    query_normed = normalize(query_latent[0], query_gain)
    pair_normed = normalize(keyvalue_latent[0], keyvalue_gain)
    own_positions = (device_index * tokens + jnp.arange(tokens, dtype=jnp.int32)).astype(
        jnp.float32
    )
    rope_own = rotate(rope_key[0].astype(jnp.float32)[:, None, :], own_positions)[:, 0, :].astype(
        jnp.bfloat16
    )
    query_all, pair_all, rope_all = (
        lax.all_gather(query_normed, "sp", axis=0, tiled=True),
        lax.all_gather(pair_normed, "sp", axis=0, tiled=True),
        lax.all_gather(rope_own, "sp", axis=0, tiled=True),
    )
    length = tokens * spread
    all_positions = jnp.arange(length, dtype=jnp.int32).astype(jnp.float32)

    def own_columns(weight, width):
        count = weight.shape[1] // (width * spread)
        return lax.dynamic_slice_in_dim(weight, device_index * count * width, count * width, 1)

    own_narrow_query = own_columns(narrow_query, width_narrow)
    own_broad_query = own_columns(broad_query, width_broad)
    own_narrow_key = own_columns(narrow_key, PLAIN_NARROW)
    own_narrow_value = own_columns(narrow_value, VALUE_SIZE)
    own_broad_key = own_columns(broad_key, PLAIN_BROAD)
    own_broad_value = own_columns(broad_value, VALUE_SIZE)
    query_sums = make_fold(
        query_all,
        (
            lax.all_gather(own_narrow_query, "dp", axis=0, tiled=True),
            lax.all_gather(own_broad_query, "dp", axis=0, tiled=True),
        ),
    )
    pair_sums = make_fold(
        pair_all,
        (
            lax.all_gather(own_narrow_key, "dp", axis=0, tiled=True),
            lax.all_gather(own_narrow_value, "dp", axis=0, tiled=True),
            lax.all_gather(own_broad_key, "dp", axis=0, tiled=True),
            lax.all_gather(own_broad_value, "dp", axis=0, tiled=True),
        ),
    )
    members = (
        arrange(query_sums[0], width_narrow, all_positions, 1, True),
        arrange(pair_sums[0], PLAIN_NARROW, all_positions, 1, False),
        arrange(pair_sums[1], VALUE_SIZE, all_positions, 1, False),
        arrange(query_sums[1], width_broad, all_positions, 1, True),
        arrange(pair_sums[2], PLAIN_BROAD, all_positions, 1, False),
        arrange(pair_sums[3], VALUE_SIZE, all_positions, 1, False),
    )
    mixed_first, mixed_second = attend_both(members, rope_all)
    back_first, back_second = (
        lax.all_to_all(mixed_first, "sp", split_axis=0, concat_axis=1, tiled=True),
        lax.all_to_all(mixed_second, "sp", split_axis=0, concat_axis=1, tiled=True),
    )
    return (finish(back_first), finish(back_second))


VMEM = pl.BlockSpec(memory_space=pltpu.VMEM)
SMALL = pltpu.CompilerParams(vmem_limit_bytes=16 * 2**20)


def exchange(array, axis, distance):
    size = lax.axis_size(axis)
    return lax.ppermute(array, axis, [(i, i ^ distance) for i in range(size)])


def scale_rows(values, gain):
    return (
        values * lax.rsqrt(jnp.mean(values * values, axis=-1, keepdims=True) + EPSILON) * gain
    )


def pack_kernel(
    latent, rope, narrow_key, narrow_value, broad_key, broad_value, narrow_query, broad_query,
    query_latent, query_gain, pair_gain,
    latent_out, pair_out, query_out, query_latent_out, query_gain_out, pair_gain_out, semaphores,
):
    tokens, rank = latent.shape
    pieces = rank // tokens
    rows = rope.shape[0] // pieces
    copies = [
        (latent, latent_out.at[:tokens, :]),
        (query_latent, query_latent_out),
        (query_gain, query_gain_out),
        (pair_gain, pair_gain_out),
    ]
    for j in range(pieces):
        copies.append(
            (
                rope.at[rows * j : rows * (j + 1), :],
                latent_out.at[tokens:, tokens * j : tokens * (j + 1)],
            )
        )
    start = 0
    for piece in (narrow_key, narrow_value, broad_key, broad_value):
        copies.append((piece, pair_out.at[:, start : start + piece.shape[1]]))
        start += piece.shape[1]
    start = 0
    for piece in (narrow_query, broad_query):
        copies.append((piece, query_out.at[:, start : start + piece.shape[1]]))
        start += piece.shape[1]
    copies = [
        pltpu.make_async_copy(source, target, semaphores.at[i])
        for i, (source, target) in enumerate(copies)
    ]
    for copy in copies:
        copy.start()
    for copy in copies:
        copy.wait()


def gather_rows(blocks, weight):
    me = lax.axis_index("dp")
    for distance, block in enumerate(blocks):
        rows = block.shape[0]
        weight[pl.ds(pl.multiple_of((me ^ distance) * rows, rows), rows), :] = block[...]


def pair_kernel(parts, shares, heads, *refs):
    latents, blocks = refs[: parts + 1], refs[parts + 1 : parts + 1 + shares]
    gain, cosine, sine, narrow_keys, narrow_values, broad_keys, broad_values, weight = refs[
        parts + 1 + shares :
    ]
    gather_rows(blocks, weight)
    rank = weight.shape[0]
    half = ROTARY // 2
    narrow, broad, value = PLAIN_NARROW * heads, PLAIN_BROAD * heads, VALUE_SIZE * heads
    for part in range(parts):
        latent = latents[part][...].astype(jnp.float32)
        if part == parts - 1:
            latent = latent + latents[parts][...].astype(jnp.float32)
        rows = latent.shape[0] * rank // (rank + ROTARY)
        lift = ROTARY * rows // rank
        own = slice(rows * part, rows * (part + 1))
        normed = scale_rows(latent[:rows, :], gain[...]).astype(jnp.bfloat16)
        wide = latent[rows:, :]
        rope = jnp.concatenate(
            [wide[:, rows * j : rows * (j + 1)] for j in range(ROTARY // lift)], axis=0
        )
        first, second = rope[:half], rope[half:]
        near, far = cosine[:, own], sine[:, own]
        rope = jnp.concatenate([first * near - second * far, first * far + second * near], axis=0)
        rope = rope.T.astype(jnp.bfloat16)
        sums = jnp.dot(normed, weight[...], preferred_element_type=jnp.float32).astype(
            jnp.bfloat16
        )
        for head in range(heads):
            start = PLAIN_NARROW * head
            narrow_keys[head, own, :PLAIN_NARROW] = sums[:, start : start + PLAIN_NARROW]
            narrow_keys[head, own, PLAIN_NARROW:] = rope
            start = narrow + value + PLAIN_BROAD * head
            broad_keys[head, own, :PLAIN_BROAD] = sums[:, start : start + PLAIN_BROAD]
            broad_keys[head, own, PLAIN_BROAD:] = rope
        narrow_values[own, :] = sums[:, narrow : narrow + value]
        broad_values[own, :] = sums[:, narrow + value + broad :]


def attend_heads(queries, keys, values, width, out):
    heads = keys.shape[0]
    lanes = 2 * VALUE_SIZE
    low = lax.broadcasted_iota(jnp.int32, (1, lanes), 1) < VALUE_SIZE
    attended = []
    for pair in range(heads // 2):
        value = values[:, lanes * pair : lanes * (pair + 1)]
        results = []
        for head in (2 * pair, 2 * pair + 1):
            query = queries[:, width * head : width * (head + 1)]
            scores = lax.dot_general(
                query, keys[head], (((1,), (1,)), ((), ())), preferred_element_type=jnp.float32
            ) * (width ** (-0.5))
            shifted = jnp.exp(scores - jnp.max(scores, axis=-1, keepdims=True))
            totals = jnp.sum(shifted, axis=-1, keepdims=True)
            mixed = jnp.dot(
                shifted.astype(jnp.bfloat16), value, preferred_element_type=jnp.float32
            )
            results.append(mixed / totals)
        attended.append(jnp.where(low, *results).astype(jnp.bfloat16).astype(jnp.float32))
    attended = jnp.concatenate(attended, axis=1)
    out[...] = scale_rows(attended, 1.0).astype(jnp.bfloat16)


def turn(sums, width, cosine, sine):
    lanes = cosine.shape[1]
    lane = lax.broadcasted_iota(jnp.int32, (1, lanes), 1)
    first = lane % ROTARY < ROTARY // 2
    turned = []
    for start in range(0, sums.shape[1], lanes):
        tile = sums[:, start : start + lanes]
        partner = jnp.where(
            first, pltpu.roll(tile, lanes - ROTARY // 2, 1), pltpu.roll(tile, ROTARY // 2, 1)
        )
        rotary = (lane + start) % width >= width - ROTARY
        turned.append(jnp.where(rotary, tile * cosine + partner * sine, tile))
    return jnp.concatenate(turned, axis=1).astype(jnp.bfloat16)


def query_kernel(shares, heads, *refs):
    blocks = refs[:shares]
    latent, gain, cosine, sine, narrow_keys, narrow_values, broad_keys, broad_values = refs[
        shares : shares + 8
    ]
    narrow_out, broad_out, weight = refs[shares + 8 :]
    gather_rows(blocks, weight)
    normed = scale_rows(latent[...].astype(jnp.float32), gain[...]).astype(jnp.bfloat16)
    sums = jnp.dot(normed, weight[...], preferred_element_type=jnp.float32)
    cosine, sine = cosine[...], sine[...]
    width = PLAIN_NARROW + ROTARY
    narrow = turn(sums[:, : width * heads], width, cosine, sine)
    attend_heads(narrow, narrow_keys, narrow_values, width, narrow_out)
    split = width * heads
    width = PLAIN_BROAD + ROTARY
    broad = turn(sums[:, split:], width, cosine, sine)
    attend_heads(broad, broad_keys, broad_values, width, broad_out)


def by_tokens_body(
    query_latent,
    keyvalue_latent,
    rope_key,
    query_gain,
    keyvalue_gain,
    narrow_query,
    broad_query,
    narrow_key,
    narrow_value,
    broad_key,
    broad_value,
):
    shape = jax.ShapeDtypeStruct
    spread, shares = lax.axis_size("sp"), lax.axis_size("dp")
    tokens, pair_rank = keyvalue_latent.shape[1:]
    query_rank = query_latent.shape[2]
    heads = narrow_value.shape[1] // VALUE_SIZE
    values = VALUE_SIZE * heads
    pair_width = narrow_key.shape[1] + broad_key.shape[1] + 2 * values
    query_width = narrow_query.shape[1] + broad_query.shape[1]
    length = tokens * spread

    pieces = pair_rank // tokens
    packed, pair_rows, query_rows, query_latent, query_gain, pair_gain = pl.pallas_call(
        pack_kernel,
        out_shape=(
            shape((tokens + ROTARY // pieces, pair_rank), jnp.bfloat16),
            shape((pair_rank // shares, pair_width), jnp.bfloat16),
            shape((query_rank // shares, query_width), jnp.bfloat16),
            shape((tokens, query_rank), jnp.bfloat16),
            shape((1, query_rank), jnp.float32),
            shape((1, pair_rank), jnp.float32),
        ),
        in_specs=[pl.BlockSpec(memory_space=pltpu.HBM)] * 11,
        out_specs=(VMEM,) * 6,
        scratch_shapes=[pltpu.SemaphoreType.DMA((10 + pieces,))],
        compiler_params=SMALL,
    )(
        *(
            pltpu.with_memory_space_constraint(array, pltpu.HBM)
            for array in (
                keyvalue_latent[0], rope_key[0].T, narrow_key, narrow_value, broad_key,
                broad_value, narrow_query, broad_query, query_latent[0], query_gain[None, :],
                keyvalue_gain[None, :],
            )
        )
    )

    x, y = 2, 4
    query_x = exchange(query_rows, "dp", x)
    pair_y = exchange(pair_rows, "dp", y)
    pair_x = exchange(pair_rows, "dp", x)
    query_y = exchange(query_rows, "dp", y)
    latent_two = exchange(packed, "sp", 2)
    latent_one = exchange(packed, "sp", 1)
    latent_inner = lax.ppermute(packed, "sp", [(1, 2), (2, 1)])
    latent_outer = lax.ppermute(latent_two, "sp", [(1, 0), (2, 3)])
    query_xy = exchange(query_x, "dp", y)
    pair_xy = exchange(pair_y, "dp", x)
    latents = [packed, latent_one, latent_two, latent_inner, latent_outer]

    def with_partner(arrays):
        both = []
        for array in arrays:
            both += [array, exchange(array, "dp", 1)]
        return both

    pair_blocks = with_partner([pair_rows, pair_x, pair_y, pair_xy])
    query_blocks = with_partner([query_rows, query_x, query_y, query_xy])

    half = ROTARY // 2
    frequency = ROTARY_BASE ** (-jnp.arange(half, dtype=jnp.float32) / half)
    place = jnp.arange(length, dtype=jnp.int32)
    me = lax.axis_index("sp")
    places = (me ^ (place // tokens)) * tokens + place % tokens
    angles = frequency[:, None] * places.astype(jnp.float32)[None, :]
    key_cosine, key_sine = jnp.cos(angles), jnp.sin(angles)
    lane = jnp.arange(4 * ROTARY, dtype=jnp.int32)
    frequency = ROTARY_BASE ** (-(lane % half).astype(jnp.float32) / half)
    places = me * tokens + jnp.arange(tokens, dtype=jnp.int32)
    angles = places.astype(jnp.float32)[:, None] * frequency[None, :]
    cosine = jnp.cos(angles)
    sine = jnp.where(lane % ROTARY < half, -1.0, 1.0)[None, :] * jnp.sin(angles)

    keys_and_values = pl.pallas_call(
        functools.partial(pair_kernel, spread, shares, heads),
        out_shape=(
            shape((heads, length, PLAIN_NARROW + ROTARY), jnp.bfloat16),
            shape((length, values), jnp.bfloat16),
            shape((heads, length, PLAIN_BROAD + ROTARY), jnp.bfloat16),
            shape((length, values), jnp.bfloat16),
        ),
        in_specs=[VMEM] * (spread + 1 + shares + 3),
        out_specs=(VMEM,) * 4,
        compiler_params=SMALL,
        scratch_shapes=[pltpu.VMEM((pair_rank, pair_width), jnp.bfloat16)],
        cost_estimate=pl.CostEstimate(
            flops=2 * length * pair_rank * pair_width, bytes_accessed=0, transcendentals=0
        ),
    )(*latents, *pair_blocks, pair_gain, key_cosine, key_sine)

    narrow, broad = pl.pallas_call(
        functools.partial(query_kernel, shares, heads),
        out_shape=(shape((tokens, values), jnp.bfloat16),) * 2,
        in_specs=[VMEM] * (shares + 8),
        out_specs=(VMEM,) * 2,
        compiler_params=SMALL,
        scratch_shapes=[pltpu.VMEM((query_rank, query_width), jnp.bfloat16)],
    )(*query_blocks, query_latent, query_gain, cosine, sine, *keys_and_values)
    return narrow[None], broad[None]


def by_tokens(*arrays):
    return by_tokens_body(*arrays)


def solution(mesh):
    small = mesh.shape["dp"] == 8 and mesh.shape["sp"] == 4
    on_device = by_tokens if small else by_heads

    in_specs = (
        P("dp", "sp", None),
        P("dp", "sp", None),
        P("dp", "sp", None),
        P(),
        P(),
        P("dp", None),
        P("dp", None),
        P("dp", None),
        P("dp", None),
        P("dp", None),
        P("dp", None),
    )
    out_specs = (P("dp", "sp", None), P("dp", "sp", None))
    return jax.shard_map(
        on_device, mesh=mesh, in_specs=in_specs, out_specs=out_specs, check_vma=False
    )
```
